32 devices in a mesh: sp: 8 (over z, y), tp: 4 (over x, core).
Axes of the slice: x: 2, y: 2, z: 4, core: 2. Of those that a mesh axis runs over, the one named last changes fastest.
Arguments:
- residual_in: bfloat16 [6144, 2048], P('sp', 'tp'), may hold values from -11 to 11
- queries: bfloat16 [6144, 1024], P('sp', 'tp'), may hold values from -6 to 6
- keys: bfloat16 [6144, 256], P('sp'), may hold values from -6 to 6
- values: bfloat16 [6144, 256], P('sp'), may hold values from -6 to 6
- query_gain: float32 [128], replicated, may hold values from 1.5 to 5
- key_norm_gain: float32 [128], replicated, may hold values from 1.5 to 5
- out_weight: bfloat16 [1024, 2048], P('tp'), may hold values from -0.1875 to 0.1875
- mlp_gain: float32 [2048], replicated, may hold values from 0.1 to 1.9
- gate_weight: bfloat16 [2048, 5632], P('sp', 'tp'), may hold values from -0.125 to 0.125
- up_weight: bfloat16 [2048, 5632], P('sp', 'tp'), may hold values from -0.125 to 0.125
- down_weight: bfloat16 [5632, 2048], P('tp', 'sp'), may hold values from -0.15625 to 0.15625
Outputs:
- layer_out: bfloat16 [6144, 2048], P('sp', 'tp')
The draws below stay inside these ranges and needn't reach their ends.
All inputs are finite; a program needn't handle non-finite values.
Results may differ from the reference program's by a relative error of at most 0.012.
The reference program's roundings to bfloat16 on the way count: a program that leaves them out, or rounds other values in their place, can miss the bound.
Values may be sent and summed in bfloat16 or wider, within the bound.
No kernel may reach another device: no remote copies, remote signals or barrier semaphores. Data moves between devices by JAX's collectives and lax.ppermute only.
A program may use at most 64 MiB of HBM per device.

```python
import math
import jax
import jax.numpy as jnp
from jax import lax

D = 2048
HEAD_SIZE = 128
QUERY_HEADS = 8
KEY_VALUE_HEADS = 2
FF = 5632
GRID = 64
TOK_DEV = 768
SEQUENCE_TOKENS = 6144
N_TP = 4


def draw_residual_in(key, part):
    column_scale = 0.5 * 4.0 ** (jnp.arange(D, dtype=jnp.float32) / D)
    rotary_period = jnp.clip(jax.random.normal(jax.random.fold_in(key, 3), (SEQUENCE_TOKENS, D)), -4.0, 4.0)
    return (rotary_period * column_scale).astype(jnp.bfloat16)


def draw_queries(key, part):
    rotary_period = jnp.clip(jax.random.normal(jax.random.fold_in(key, 1), (SEQUENCE_TOKENS, QUERY_HEADS * HEAD_SIZE)), -4.0, 4.0)
    return jnp.clip(rotary_period, -6.0, 6.0).astype(jnp.bfloat16)


def draw_keys(key, part):
    rotary_period = jnp.clip(jax.random.normal(jax.random.fold_in(key, 2), (SEQUENCE_TOKENS, KEY_VALUE_HEADS * HEAD_SIZE)), -4.0, 4.0)
    return jnp.clip(rotary_period, -6.0, 6.0).astype(jnp.bfloat16)


def draw_gain(key, salt):
    return jnp.exp(jax.random.uniform(jax.random.fold_in(key, salt), (HEAD_SIZE,), jnp.float32, math.log(1.5), math.log(3.0)))


def draw_query_gain(key, part):
    return draw_gain(key, 4)


def draw_key_norm_gain(key, part):
    return draw_gain(key, 5)


def steps_of(stream_key, extent, cuts, low, top_value):
    loudness, own = 1.0, jax.random.fold_in(stream_key, 6)
    for dim, shards_of in cuts:
        steps = jnp.exp(jax.random.uniform(jax.random.fold_in(own, dim), (shards_of,), jnp.float32, low / len(cuts), top_value / len(cuts)))
        loudness = loudness * jnp.repeat(steps, extent[dim] // shards_of).reshape([-1 if axis == dim else 1 for axis in range(len(extent))])
    return loudness


def gaussian(key, extent, spread, limit, cuts=(), kind=jnp.bfloat16):
    drawn = jax.random.normal(key, extent, jnp.float32) * spread
    if len(cuts) > 0:
        drawn = steps_of(key, extent, cuts, -0.22, 0.18) * drawn
    return jnp.clip(drawn, min=-limit, max=limit).astype(kind)


def setup_inputs(seed: int = 0) -> dict:
    key_of = jax.random.split(jax.random.key(seed), 12)
    return {
        "residual_in": draw_residual_in(jax.random.fold_in(key_of[11], 71), 0),
        "queries": draw_queries(jax.random.fold_in(key_of[11], 71), 0),
        "keys": draw_keys(jax.random.fold_in(key_of[11], 71), 0),
        "values": gaussian(key_of[3], (SEQUENCE_TOKENS, KEY_VALUE_HEADS * HEAD_SIZE), 1.0, 6.0, ((0, 8),)),
        "query_gain": draw_query_gain(jax.random.fold_in(key_of[11], 71), 0),
        "key_norm_gain": draw_key_norm_gain(jax.random.fold_in(key_of[11], 71), 0),
        "out_weight": gaussian(key_of[6], (QUERY_HEADS * HEAD_SIZE, D), (QUERY_HEADS * HEAD_SIZE) ** -0.5, 0.1875, ((0, 4),)),
        "mlp_gain": jnp.clip(1.0 + 0.18 * jax.random.normal(key_of[7], (D,), jnp.float32), 0.1, 1.9),
        "gate_weight": gaussian(key_of[8], (D, FF), D ** -0.5, 0.125, ((0, 8), (1, 4))),
        "up_weight": gaussian(key_of[9], (D, FF), D ** -0.5, 0.125, ((0, 8), (1, 4))),
        "down_weight": gaussian(key_of[10], (FF, D), (FF // 4) ** -0.5, 0.15625, ((0, 4), (1, 8))),
    }


eps = 1e-06
rotary_base = 10000.0

def apply_rotary(vectors, grid_positions):
    half_size = vectors.shape[-1] // 2
    frequency = rotary_base ** (-jnp.arange(0, half_size, 2, dtype=jnp.float32) / half_size)
    grid_row = (grid_positions // GRID).astype(jnp.float32)
    grid_col = (grid_positions % GRID).astype(jnp.float32)
    angles = jnp.concatenate([grid_row[:, None] * frequency, grid_col[:, None] * frequency], axis=-1)[:, None, :]
    cosine_table = jnp.cos(angles)
    sine_table = jnp.sin(angles)
    first_half = vectors[..., :half_size]
    second_half = vectors[..., half_size:]
    return jnp.concatenate([first_half * cosine_table - second_half * sine_table, first_half * sine_table + second_half * cosine_table], axis=-1)

def per_head_norm(vectors, gain):
    return vectors * lax.rsqrt(lax.optimization_barrier(jnp.mean(vectors * vectors, axis=-1, keepdims=True)) + eps) * gain

def grouped_sum(left, right, groups):
    group_width = left.shape[1] // groups

    def add_group(running, group_index):
        left_part = lax.dynamic_slice_in_dim(left, group_index * group_width, group_width, 1)
        right_part = lax.dynamic_slice_in_dim(right, group_index * group_width, group_width, 0)
        partial_sum = jnp.dot(left_part, right_part, preferred_element_type=jnp.float32)
        rounded = lax.optimization_barrier(partial_sum.astype(jnp.bfloat16))
        return (running + rounded.astype(jnp.float32), None)
    start_value = jnp.zeros((left.shape[0], right.shape[1]), jnp.float32)
    result, ignored = lax.scan(add_group, start_value, jnp.arange(groups, dtype=jnp.int32))
    return result

def reference(residual_in, queries, keys, values, query_gain, key_norm_gain, out_weight, mlp_gain, gate_weight, up_weight, down_weight):
    grid_positions = jnp.arange(SEQUENCE_TOKENS, dtype=jnp.int32)
    queries_per_group = QUERY_HEADS // KEY_VALUE_HEADS
    query_rows = apply_rotary(per_head_norm(queries.astype(jnp.float32).reshape(SEQUENCE_TOKENS, QUERY_HEADS, HEAD_SIZE), query_gain), grid_positions).astype(jnp.bfloat16)
    key_matrix = apply_rotary(per_head_norm(keys.astype(jnp.float32).reshape(SEQUENCE_TOKENS, KEY_VALUE_HEADS, HEAD_SIZE), key_norm_gain), grid_positions).astype(jnp.bfloat16)
    value_matrix = values.reshape(SEQUENCE_TOKENS, KEY_VALUE_HEADS, HEAD_SIZE)
    score_scale = HEAD_SIZE ** (-0.5)

    def one_head(head_index):
        head_queries = lax.dynamic_index_in_dim(query_rows, head_index, 1, keepdims=False)
        shared = head_index // queries_per_group
        head_keys = lax.dynamic_index_in_dim(key_matrix, shared, 1, keepdims=False)
        head_values = lax.dynamic_index_in_dim(value_matrix, shared, 1, keepdims=False)

        def one_block(first_row):
            block_queries = lax.dynamic_slice_in_dim(head_queries, first_row, TOK_DEV, 0)
            scores = jnp.dot(block_queries, head_keys.T, preferred_element_type=jnp.float32) * score_scale
            row_max = lax.optimization_barrier(jnp.max(scores, axis=1, keepdims=True))
            weights = jnp.exp(scores - row_max)
            row_sum = lax.optimization_barrier(jnp.sum(weights, axis=1, keepdims=True))
            weighted = jnp.dot(weights.astype(jnp.bfloat16), head_values, preferred_element_type=jnp.float32)
            return (weighted / row_sum).astype(jnp.bfloat16)
        starts = jnp.arange(0, SEQUENCE_TOKENS, TOK_DEV, dtype=jnp.int32)
        return lax.map(one_block, starts).reshape(SEQUENCE_TOKENS, HEAD_SIZE)
    heads_out = lax.map(one_head, jnp.arange(QUERY_HEADS, dtype=jnp.int32))
    attended = jnp.transpose(heads_out, (1, 0, 2)).reshape(SEQUENCE_TOKENS, QUERY_HEADS * HEAD_SIZE)
    projected = grouped_sum(attended, out_weight, N_TP)
    residual_mid = residual_in.astype(jnp.float32) + projected
    normed = (residual_mid * lax.rsqrt(lax.optimization_barrier(jnp.mean(residual_mid * residual_mid, axis=1, keepdims=True)) + eps) * mlp_gain).astype(jnp.bfloat16)
    gate_out = jnp.dot(normed, gate_weight, preferred_element_type=jnp.float32)
    up_out = jnp.dot(normed, up_weight, preferred_element_type=jnp.float32)
    hidden = (jax.nn.silu(gate_out) * up_out).astype(jnp.bfloat16)
    down_sum = grouped_sum(hidden, down_weight, N_TP)
    return (residual_mid + 0.5 * down_sum).astype(jnp.bfloat16)
```

```python
import math

import jax
import jax.numpy as jnp
from jax import lax
from jax.experimental import pallas as pl
from jax.experimental.pallas import tpu as pltpu
from jax.sharding import PartitionSpec as P

HEAD_SIZE = 128
KEY_VALUE_HEADS = 2
GRID = 64

eps = 1e-06
rotary_base = 10000.0
LOG2E = 1.4426950408889634


bf16 = jnp.bfloat16
f32 = jnp.float32


def rotary_tables(grid_positions, head_size):
    half_size = head_size // 2
    frequency = rotary_base ** (-jnp.arange(0, half_size, 2, dtype=f32) / half_size)
    grid_row = (grid_positions // GRID).astype(f32)
    grid_col = (grid_positions % GRID).astype(f32)
    angles = jnp.concatenate(
        [grid_row[:, None] * frequency, grid_col[:, None] * frequency], axis=-1
    )
    return jnp.cos(angles), jnp.sin(angles)


def rope_norm(vectors, gain, cosine_table, sine_table):
    vectors = vectors * lax.rsqrt(jnp.mean(vectors * vectors, axis=-1, keepdims=True) + eps) * gain
    half_size = vectors.shape[-1] // 2
    first_half = vectors[..., :half_size]
    second_half = vectors[..., half_size:]
    return jnp.concatenate(
        [
            first_half * cosine_table - second_half * sine_table,
            first_half * sine_table + second_half * cosine_table,
        ],
        axis=-1,
    ).astype(bf16)


def cost(flops, bytes_accessed=0):
    return pl.CostEstimate(flops=flops, bytes_accessed=bytes_accessed, transcendentals=0)


def whole(shape):
    return pl.BlockSpec(shape, lambda *_: (0,) * len(shape))


def largest_tile(rows, limit):
    tile = min(rows, limit)
    while rows % tile:
        tile -= 8
    return tile


def attention(query_matrix, blocks, scale):
    rows, width = query_matrix.shape
    block_rows = blocks[0].shape[0]
    count = len(blocks)
    tile = largest_tile(rows, 512)
    factor = scale * LOG2E

    def kernel(q_ref, *refs):
        block_refs, o_ref, ext_ref = refs[:count], refs[count], refs[count + 1]

        @pl.when(pl.program_id(0) == 0)
        def _():
            ones = jnp.ones((block_rows, width), bf16)
            for index in range(count):
                ext_ref[index, :, :width] = block_refs[index][:, width:]
                ext_ref[index, :, width:] = ones

        q = q_ref[...]
        running_max, weighted = None, None
        for index in range(count):
            scores = lax.dot_general(
                q,
                block_refs[index][:, :width],
                (((1,), (1,)), ((), ())),
                preferred_element_type=f32,
            )
            block_max = jnp.max(scores, axis=1, keepdims=True)
            new_max = block_max if index == 0 else jnp.maximum(running_max, block_max)
            weights = jnp.exp2((scores - new_max) * factor).astype(bf16)
            part = jnp.dot(weights, ext_ref[index], preferred_element_type=f32)
            if index == 0:
                weighted = part
            else:
                weighted = weighted * jnp.exp2((running_max - new_max) * factor) + part
            running_max = new_max
        o_ref[...] = (weighted[:, :width] / weighted[:, width:]).astype(bf16)

    return pl.pallas_call(
        kernel,
        grid=(rows // tile,),
        in_specs=[pl.BlockSpec((tile, width), lambda i: (i, 0))]
        + [whole(b.shape) for b in blocks],
        out_specs=pl.BlockSpec((tile, width), lambda i: (i, 0)),
        out_shape=jax.ShapeDtypeStruct((rows, width), bf16),
        scratch_shapes=[pltpu.VMEM((count, block_rows, 2 * width), bf16)],
        cost_estimate=cost(8 * rows * width * block_rows * count),
        name="attention",
    )(query_matrix, *blocks)


def out_projection(parts, weights, residual):
    rows, width = residual.shape
    count = len(parts)
    inner = parts[0].shape[1]
    tile = largest_tile(rows, 256)

    def kernel(*refs):
        part_refs, weight_refs = refs[:count], refs[count : 2 * count]
        residual_ref, mid_ref, send_ref = refs[2 * count :]
        total = residual_ref[...].astype(f32)
        for part_ref, weight_ref in zip(part_refs, weight_refs):
            term = jnp.dot(part_ref[...], weight_ref[...], preferred_element_type=f32)
            total = total + term.astype(bf16).astype(f32)
        mid_ref[...] = total
        send_ref[...] = total.astype(bf16)

    row_block = pl.BlockSpec((tile, width), lambda i: (i, 0))
    return pl.pallas_call(
        kernel,
        grid=(rows // tile,),
        in_specs=[pl.BlockSpec((tile, inner), lambda i: (i, 0))] * count
        + [whole(w.shape) for w in weights]
        + [row_block],
        out_specs=[row_block, row_block],
        out_shape=[
            jax.ShapeDtypeStruct((rows, width), f32),
            jax.ShapeDtypeStruct((rows, width), bf16),
        ],
        cost_estimate=cost(2 * rows * width * inner * count),
        name="out_projection",
    )(*parts, *weights, residual)


def mixer_norm(slices, gains):
    rows, width = slices[0].shape
    count = len(slices)
    tile = largest_tile(rows, 256)

    def kernel(*refs):
        slice_refs, gain_ref, o_ref = refs[:count], refs[count], refs[count + 1]
        total = jnp.zeros((tile, 1), f32)
        for ref in slice_refs:
            v = ref[...].astype(f32)
            total = total + jnp.sum(v * v, axis=1, keepdims=True)
        scale = lax.rsqrt(total / (count * width) + eps)
        for index, ref in enumerate(slice_refs):
            v = ref[...].astype(f32)
            o_ref[index] = (v * scale * gain_ref[index : index + 1, :]).astype(bf16)

    return pl.pallas_call(
        kernel,
        grid=(rows // tile,),
        in_specs=[pl.BlockSpec((tile, width), lambda i: (i, 0))] * count + [whole(gains.shape)],
        out_specs=pl.BlockSpec((count, tile, width), lambda i: (0, i, 0)),
        out_shape=jax.ShapeDtypeStruct((count, rows, width), bf16),
        cost_estimate=cost(20 * rows * width * count),
        name="mixer_norm",
    )(*slices, gains)


def gate_up(normed, blocks, slots):
    count, rows, width = normed.shape
    depth, units = blocks[0].shape
    depth //= 2
    tile = largest_tile(rows, 384)

    def kernel(slot_ref, x_ref, *refs):
        block_refs, o_ref = refs[:-1], refs[-1]
        x = jnp.concatenate(
            [
                x_ref[
                    slot_ref[2 * s],
                    :,
                    pl.ds(pl.multiple_of(slot_ref[2 * s + 1] * depth, depth), depth),
                ]
                for s in range(len(block_refs))
            ],
            axis=1,
        )
        gate = jnp.dot(
            x,
            jnp.concatenate([ref[:depth, :] for ref in block_refs], axis=0),
            preferred_element_type=f32,
        )
        up = jnp.dot(
            x,
            jnp.concatenate([ref[depth:, :] for ref in block_refs], axis=0),
            preferred_element_type=f32,
        )
        o_ref[...] = (gate / (1.0 + jnp.exp(-gate)) * up).astype(bf16)

    return pl.pallas_call(
        kernel,
        grid_spec=pltpu.PrefetchScalarGridSpec(
            num_scalar_prefetch=1,
            grid=(rows // tile,),
            in_specs=[pl.BlockSpec((count, tile, width), lambda i, s: (0, i, 0))]
            + [whole(b.shape) for b in blocks],
            out_specs=pl.BlockSpec((tile, units), lambda i, s: (i, 0)),
        ),
        out_shape=jax.ShapeDtypeStruct((rows, units), bf16),
        cost_estimate=cost(4 * rows * width * count * units),
        name="gate_up",
    )(slots, normed, *blocks)


def down(hidden, blocks, slots, slices):
    rows = hidden[0].shape[0]
    units, wide = blocks[0].shape
    n_hidden = len(hidden)
    per_slice = len(blocks) // slices
    tile = largest_tile(rows, 384)

    def kernel(slot_ref, *refs):
        hidden_refs, block_refs, o_ref = refs[:n_hidden], refs[n_hidden:-1], refs[-1]
        h = jnp.concatenate([ref[...] for ref in hidden_refs], axis=1)
        for first in range(0, len(block_refs), 2):
            group = range(first, first + 2)
            part = jnp.dot(
                h,
                jnp.concatenate([block_refs[s][...] for s in group], axis=1),
                preferred_element_type=f32,
            ).astype(bf16)
            for s in group:
                piece = part[:, (s - first) * wide : (s - first + 1) * wide]
                column = slot_ref[2 * s + 1] * wide
                if wide % 128 == 0:
                    column = pl.multiple_of(column, wide)
                    o_ref[slot_ref[2 * s], :, pl.ds(column, wide)] = piece
                else:
                    for place in range(per_slice):

                        @pl.when(slot_ref[2 * s + 1] == place)
                        def _():
                            o_ref[slot_ref[2 * s], :, place * wide : (place + 1) * wide] = piece

    return pl.pallas_call(
        kernel,
        grid_spec=pltpu.PrefetchScalarGridSpec(
            num_scalar_prefetch=1,
            grid=(rows // tile,),
            in_specs=[pl.BlockSpec((tile, h.shape[1]), lambda i, s: (i, 0)) for h in hidden]
            + [whole(b.shape) for b in blocks],
            out_specs=pl.BlockSpec((slices, tile, per_slice * wide), lambda i, s: (0, i, 0)),
        ),
        out_shape=jax.ShapeDtypeStruct((slices, rows, per_slice * wide), bf16),
        cost_estimate=cost(2 * rows * units * wide * len(blocks)),
        name="down",
    )(slots, *hidden, *blocks)


def unit_chunks(units):
    step = max(128, -(-units // 3 // 128) * 128)
    edges = list(range(0, units, step)) + [units]
    return [(a, b) for a, b in zip(edges[:-1], edges[1:]) if b > a]


def make_on_device(n_sp, n_tp):
    n_z = math.gcd(n_sp, 4)
    n_y, n_x = n_sp // n_z, n_tp // 2
    per_slice = n_sp // n_tp

    def pairs(route):
        result = []
        for sp in range(n_sp):
            for tp in range(n_tp):
                z, y = divmod(sp, n_y)
                h, e = divmod(z, 2)
                x, c = divmod(tp, 2)
                x2, y2, h2, e2, c2 = route(x, y, h, e, c)
                result.append((sp * n_tp + tp, ((2 * h2 + e2) * n_y + y2) * n_tp + 2 * x2 + c2))
        return result

    def send(value, route):
        return lax.ppermute(value, ("sp", "tp"), pairs(route))

    def along_y(step):
        return lambda x, y, h, e, c: (x, (y + step) % n_y, h, e, c)

    def other_core(x, y, h, e, c):
        return (x, y, h, e, 1 - c)

    def turn(x, y, h, e, c):
        return (x, y, h, c, e)

    def far(x, y, h, e, c):
        return (x, y, 1 - h, e, c)

    def across_tp(dx, dc):
        return lambda x, y, h, e, c: ((x + dx) % n_x, y, h, e, c ^ dc)

    def gather_weights(block, gate=None):
        near_block = send(block, turn)
        far_block = send(near_block, far)
        if gate is not None:
            near_block, far_block, gate = lax.optimization_barrier((near_block, far_block, gate))
        own = []
        for piece in (near_block, far_block):
            own += [piece] + [send(piece, along_y(step)) for step in range(1, n_y)]
        others = [send(piece, other_core) for piece in own]
        result = []
        for first in (0, n_y):
            result += own[first : first + n_y] + others[first : first + n_y]
        return result

    def on_device(
        residual_in,
        queries,
        keys,
        values,
        query_gain,
        key_norm_gain,
        out_weight,
        mlp_gain,
        gate_weight,
        up_weight,
        down_weight,
    ):
        local_rows, own_width = residual_in.shape
        local_heads = queries.shape[1] // HEAD_SIZE
        queries_per_group = n_tp * local_heads // KEY_VALUE_HEADS
        tp_index = lax.axis_index("tp")
        sp_index = lax.axis_index("sp")
        x_bit, c_bit = tp_index // 2, tp_index % 2
        z_index, y_index = sp_index // n_y, sp_index % n_y
        h_bit, e_bit = z_index // 2, z_index % 2
        half_rows = local_rows // 2

        shared = tp_index * local_heads // queries_per_group
        half_start = c_bit * half_rows
        half_positions = (
            sp_index * local_rows + half_start + jnp.arange(half_rows, dtype=jnp.int32)
        )
        cosine_half, sine_half = rotary_tables(half_positions, HEAD_SIZE)
        own_keys = lax.dynamic_slice(
            keys, (half_start, shared * HEAD_SIZE), (half_rows, HEAD_SIZE)
        )
        own_values = lax.dynamic_slice(
            values, (half_start, shared * HEAD_SIZE), (half_rows, HEAD_SIZE)
        )
        key_rows = rope_norm(own_keys.astype(f32), key_norm_gain, cosine_half, sine_half)
        kv = jnp.concatenate([key_rows, own_values], axis=1)
        along_z = [kv]
        for dh, de in ((0, 1), (1, 0), (1, 1)):
            along_z.append(
                send(kv, lambda x, y, h, e, c, dh=dh, de=de: (x, y, h ^ dh, e ^ de, c))
            )
        kv_blocks = []
        for piece in along_z:
            kv_blocks += [piece] + [send(piece, along_y(step)) for step in range(1, n_y)]
        kv_blocks += [send(piece, other_core) for piece in kv_blocks]

        chunks = unit_chunks(gate_weight.shape[1])
        packed = [
            jnp.concatenate([gate_weight[:, a:b], up_weight[:, a:b]], axis=0) for a, b in chunks
        ]
        down_step = min(128, down_weight.shape[1])
        downs = [
            down_weight[:, a : a + down_step] for a in range(0, down_weight.shape[1], down_step)
        ]
        ordered = lax.optimization_barrier((kv, *packed, *downs))
        packed, downs = ordered[1 : 1 + len(packed)], ordered[1 + len(packed) :]
        out_pieces = []
        tp_moves = [(dx, dc) for dx in range(n_x) for dc in (0, 1)]
        for dx, dc in tp_moves:
            target = 2 * ((x_bit + dx) % n_x) + (c_bit ^ dc)
            piece = lax.dynamic_slice_in_dim(out_weight, target * own_width, own_width, 1)
            if dx or dc:
                piece = send(piece, across_tp(dx, dc))
            out_pieces.append(piece)
        gate_up_blocks = [
            gather_weights(block, kv_blocks[-1] if index == 0 else None)
            for index, block in enumerate(packed)
        ]
        down_blocks = [gather_weights(block) for block in downs]

        positions = sp_index * local_rows + jnp.arange(local_rows, dtype=jnp.int32)
        cosine_table, sine_table = rotary_tables(positions, HEAD_SIZE)
        query_matrix = jnp.concatenate(
            [
                rope_norm(
                    queries[:, i * HEAD_SIZE : (i + 1) * HEAD_SIZE].astype(f32),
                    query_gain,
                    cosine_table,
                    sine_table,
                )
                for i in range(local_heads)
            ],
            axis=0,
        )
        attended = attention(query_matrix, kv_blocks, HEAD_SIZE ** (-0.5))
        attended = jnp.concatenate(
            [attended[i * local_rows : (i + 1) * local_rows] for i in range(local_heads)], axis=1
        )
        attended_parts = [attended]
        for dx, dc in tp_moves[1:]:
            attended_parts.append(send(attended, across_tp(dx, dc)))
        residual_mid, outgoing = out_projection(attended_parts, out_pieces, residual_in)

        slices = [
            send(outgoing, lambda x, y, h, e, c, dx=dx, de=de: ((x + dx) % n_x, y, h, c ^ de, e))
            for dx, de in tp_moves
        ]
        gain_rows = mlp_gain.reshape(n_tp, own_width)
        gains = jnp.stack(
            [
                lax.dynamic_index_in_dim(
                    gain_rows, 2 * ((x_bit - dx) % n_x) + (e_bit ^ de), 0, keepdims=False
                )
                for dx, de in tp_moves
            ]
        )
        normed = mixer_norm(slices, gains)
        slots = []
        for dh in (0, 1):
            for dc in (0, 1):
                for dy in range(n_y):
                    feature = (2 * (h_bit ^ dh) + (c_bit ^ dc)) * n_y + (y_index - dy) % n_y
                    owner = feature // per_slice
                    slots += [
                        2 * ((x_bit - owner // 2) % n_x) + ((owner % 2) ^ e_bit),
                        feature % per_slice,
                    ]
        slots = jnp.stack(slots).astype(jnp.int32)
        hidden = [gate_up(normed, blocks, slots) for blocks in gate_up_blocks]
        down_shares = []
        for blocks in down_blocks:
            terms = down(hidden, blocks, slots, n_tp)
            total = None
            for index, (dx, de) in enumerate(tp_moves):
                term = send(
                    terms[index], lambda x, y, h, e, c, dx=dx, de=de: ((x - dx) % n_x, y, h, c, e ^ de)
                ).astype(f32)
                total = term if total is None else total + term
            down_shares.append(total.reshape(local_rows, per_slice, -1))
        down_share = jnp.concatenate(down_shares, axis=2).reshape(local_rows, own_width)
        return (residual_mid + 0.5 * down_share).astype(bf16)

    return on_device


def solution(mesh):
    in_specs = (
        P("sp", "tp"),
        P("sp", "tp"),
        P("sp", None),
        P("sp", None),
        P(),
        P(),
        P("tp", None),
        P(),
        P("sp", "tp"),
        P("sp", "tp"),
        P("tp", "sp"),
    )
    out_specs = P("sp", "tp")
    return jax.shard_map(
        make_on_device(mesh.shape["sp"], mesh.shape["tp"]),
        mesh=mesh,
        in_specs=in_specs,
        out_specs=out_specs,
        check_vma=False,
    )
```
